256 devices in a mesh: grp: 2 (over y), ep: 32 (over z, core), tp: 4 (over x).
Axes of the slice: x: 4, y: 2, z: 16, core: 2. Of those that a mesh axis runs over, the one named last changes fastest.
The devices are a block of a 4x16x16 slice.
Arguments:
- query_plain: bfloat16 [16384, 512], P(('grp', 'ep'), 'tp'), parts along dimension 0, may hold values from -400 to 400
- query_rotary: bfloat16 [16384, 256], P(('grp', 'ep'), 'tp'), parts along dimension 0, may hold values from -6 to 6
- latent_input: bfloat16 [16384, 256], P(('grp', 'ep')), parts along dimension 0, may hold values from -6 to 6
- rotary_key: bfloat16 [16384, 32], P(('grp', 'ep')), parts along dimension 0, may hold values from -6 to 6
- key_weight: bfloat16 [256, 512], P(None, 'tp'), may hold values from -0.375 to 0.375
- value_weight: bfloat16 [256, 512], P(None, 'tp'), may hold values from -0.375 to 0.375
- latent_gain: bfloat16 [256], replicated, may hold values from 0.099609375 to 1.8984375
- head_gain: bfloat16 [512], P('tp'), may hold values from 0.099609375 to 1.8984375
- out_weight: bfloat16 [512, 2048], P('tp'), may hold values from -0.25 to 0.25
- expert_input: bfloat16 [32768, 2048], P(('grp', 'ep', 'tp')), parts along dimension 0, may hold values from -6 to 6
- expert_gain: bfloat16 [2048], replicated, may hold values from 0.099609375 to 1.8984375
- routes: int32 [32768, 2], P(('grp', 'ep', 'tp')), parts along dimension 0, may hold values from 0 to 31, all different within a row; in each aligned block of 128 rows (0 to 127, 128 to 255, ...) at most 9 rows name the same one
- route_weight: float32 [32768, 2], P(('grp', 'ep', 'tp')), parts along dimension 0, may hold values from 0.1 to 1
- gate_weight: bfloat16 [32, 2048, 3584], P('ep', None, 'tp'), may hold values from -0.125 to 0.125
- up_weight: bfloat16 [32, 2048, 3584], P('ep', None, 'tp'), may hold values from -0.125 to 0.125
- down_weight: bfloat16 [32, 3584, 2048], P('ep', 'tp'), may hold values from -0.09375 to 0.09375
Outputs:
- attended: bfloat16 [16384, 2048], P(('grp', 'ep', 'tp')), parts along dimension 0
- expert_out: bfloat16 [32768, 2048], P(('grp', 'ep', 'tp')), parts along dimension 0
The draws below stay inside these ranges and needn't reach their ends.
There are 2 independent parts, one for each index of `grp`. The reference program is written for one: setup_inputs(seed, part) draws one part's arguments, and reference() takes and returns one part's arrays. A program takes and returns all parts, laid end to end along the dimension named above; an argument that names none is the same for every part. Nothing has to cross between parts.
Inputs may be any that keep to these rules, and one draw needn't show every extreme that they name: `routes`: each of the 128 rows of one device names 2 different experts; no expert is named by more than 9 rows of one device, a bound that some block reaches of some device.
All inputs are finite; a program needn't handle non-finite values.
Results may differ from the reference program's by a relative error of at most 0.012.
Values may be sent and summed in bfloat16 or wider, within the bound.
No kernel may reach another device: no remote copies, remote signals or barrier semaphores. Data moves between devices by JAX's collectives and lax.ppermute only.
A program may use at most 128 MiB of HBM per device.

```python
import math
import jax
import jax.numpy as jnp
import numpy as np
from jax import lax

D = 2048
HEADS = 8
PLAIN_DIM = 64
ROTARY_DIM = 32
VALUE_DIM = 64
LATENT = 256
FF = 3584
TOP = 2
TOK_A = 256
TOK_B = 128
EXPERTS = 32
CAP = 9
TOKENS_A = 8192
TOKENS_B = 16384
N_EP = 32
N_TP = 4


def draw_query_plain(key, part):
    first = jax.random.fold_in(key, 0)
    shape = (TOKENS_A, HEADS * PLAIN_DIM)
    return jnp.clip(jax.random.normal(first, shape, jnp.float32), -5.0, 5.0).astype(jnp.bfloat16)


def block_levels(key, dims, shards, least, largest):
    def one(axis_at, parts):
        steps = jax.random.uniform(jax.random.fold_in(jax.random.fold_in(key, 6), axis_at), (parts,), jnp.float32, least / len(shards), largest / len(shards))
        return jnp.repeat(jnp.exp(steps), dims[axis_at] // parts).reshape((-1,) + (1,) * (len(dims) - axis_at - 1))

    loudness = one(*shards[0])
    for cut in shards[1:]:
        loudness = loudness * one(*cut)
    return loudness


def deal_out(stream_key, own, number, rows, number_of, top, limit, slope):
    ranking = jax.random.permutation(stream_key, number_of)
    crowded, ordinary = portions_of(number_of, rows * top, limit, slope, True), portions_of(number_of, rows * top, limit, slope, False)
    places = jnp.arange(number_of)

    def named(sizes, rotation):
        used = int((sizes > 0).sum())
        fixed = max(1, used // 4)
        shifted = fixed + (places - fixed + rotation * (used - fixed)) % max(1, number_of - fixed)
        return jnp.zeros((number_of,), jnp.int32).at[ranking[jnp.where(places < fixed, places, shifted)]].set(jnp.asarray(sizes, jnp.int32))

    sizes = jnp.where(number % 4 == 0, named(crowded, number // 4), named(ordinary, number - number // 4 - 1))
    mixed = jax.random.permutation(jax.random.fold_in(own, 3), number_of)
    donor, sink = mixed[0:number_of // 2 * 2:2], mixed[1:number_of // 2 * 2:2]
    slack = jnp.minimum(sizes[donor] - 1, limit - sizes[sink]) // 2
    slack = jnp.where((donor == ranking[0]) | (sink == ranking[0]) | (sizes[sink] == 0), 0, jnp.maximum(slack, 0))
    shifted = jax.random.randint(jax.random.fold_in(own, 4), (number_of // 2,), 0, 1 << 20) % (slack + 1)
    sizes = sizes.at[donor].add(-shifted).at[sink].add(shifted)
    items = jnp.searchsorted(jnp.cumsum(sizes), jnp.arange(rows * top), side="right").astype(jnp.int32)
    grid = items.reshape(top, rows).T
    grid = grid[jax.random.permutation(jax.random.fold_in(own, 1), rows)]
    rotation = jax.random.randint(jax.random.fold_in(own, 2), (rows, 1), 0, top)
    return jnp.take_along_axis(grid, (jnp.arange(top)[None, :] + rotation) % top, axis=1)


def portions_of(number_of, total, limit, lean, full):
    loads = [(1 << 20) // math.isqrt(standing ** lean) + 1 for standing in range(1, number_of + 1)]
    largest = limit if full else min(limit, max(-(-total // number_of), total * loads[0] // sum(loads)))
    least = 1 if total - largest >= number_of - 1 else 0
    holding, rest = [largest] + [least] * (number_of - 1), total - largest - least * (number_of - 1)
    while rest > 0:
        free = [i for i in range(1, number_of) if holding[i] < largest] or [i for i in range(1, number_of) if holding[i] < limit]
        whole, budget = sum([loads[i] for i in free]), rest
        for i in free:
            extra = min(limit - holding[i], max(1, budget * loads[i] // whole), rest)
            holding[i] = holding[i] + extra
            rest = rest - extra
    return np.array(holding)


def normal_values(key, extent, scale, reach, pieces=(), kind=jnp.bfloat16):
    array = jax.random.normal(key, extent, jnp.float32) * scale
    if len(pieces) > 0:
        array = block_levels(key, extent, pieces, -0.22, 0.18) * array
    return jnp.clip(array, min=-reach, max=reach).astype(kind)


def setup_inputs(seed: int = 0, part: int = 0) -> dict:
    arg_keys = jax.random.split(jax.random.key(seed), 17)
    part_splits = jax.random.split(jax.random.fold_in(arg_keys[16], part), 17)
    query_plain = draw_query_plain(jax.random.fold_in(jax.random.fold_in(arg_keys[16], part), 71), part)
    query_rotary = normal_values(part_splits[1], (TOKENS_A, HEADS * ROTARY_DIM), 1.0, 6.0, ((0, 32), (1, 4)))
    latent_input = normal_values(part_splits[2], (TOKENS_A, LATENT), 1.0, 6.0, ((0, 32),))
    rotary_key = normal_values(part_splits[3], (TOKENS_A, ROTARY_DIM), 1.0, 6.0, ((0, 32),))
    key_weight = normal_values(arg_keys[4], (LATENT, HEADS * PLAIN_DIM), LATENT ** -0.5, 0.375, ((1, 4),))
    value_weight = normal_values(arg_keys[5], (LATENT, HEADS * VALUE_DIM), LATENT ** -0.5, 0.375, ((1, 4),))
    latent_gain = jnp.clip(1.0 + 0.18 * jax.random.normal(arg_keys[6], (LATENT,), jnp.float32), 0.099609375, 1.8984375).astype(jnp.bfloat16)
    head_gain = jnp.clip(1.0 + 0.18 * jax.random.normal(arg_keys[7], (HEADS * VALUE_DIM,), jnp.float32), 0.099609375, 1.8984375).astype(jnp.bfloat16)
    out_weight = normal_values(arg_keys[8], (HEADS * VALUE_DIM, D), (HEADS * VALUE_DIM) ** -0.5, 0.25, ((0, 4),))
    expert_input = normal_values(part_splits[9], (TOKENS_B, D), 1.0, 6.0, ((0, 128),))
    expert_gain = jnp.clip(1.0 + 0.18 * jax.random.normal(arg_keys[10], (D,), jnp.float32), 0.099609375, 1.8984375).astype(jnp.bfloat16)
    routes_keys = jax.random.split(jax.random.fold_in(part_splits[11], 1), TOKENS_B // TOK_B)
    routes_turns = jax.random.permutation(jax.random.fold_in(part_splits[11], 3), TOKENS_B // TOK_B)
    routes = jax.vmap(lambda own, number: deal_out(jax.random.fold_in(part_splits[11], 2), own, number, TOK_B, EXPERTS, TOP, CAP, 1))(routes_keys, routes_turns).reshape((TOKENS_B, TOP))
    route_weight = jnp.clip(0.1 + 0.9 * jax.random.uniform(part_splits[12], (TOKENS_B, TOP), jnp.float32) ** block_levels(part_splits[12], (TOKENS_B, TOP), ((0, 128),), -0.2, 0.2), 0.1, 1.0)
    gate_weight = normal_values(arg_keys[13], (EXPERTS, D, FF), D ** -0.5, 0.125, ((0, 32), (2, 4)))
    up_weight = normal_values(arg_keys[14], (EXPERTS, D, FF), D ** -0.5, 0.125, ((0, 32), (2, 4)))
    down_weight = normal_values(arg_keys[15], (EXPERTS, FF, D), FF ** -0.5, 0.09375, ((0, 32), (1, 4)))
    return dict(query_plain=query_plain, query_rotary=query_rotary, latent_input=latent_input, rotary_key=rotary_key, key_weight=key_weight, value_weight=value_weight, latent_gain=latent_gain, head_gain=head_gain, out_weight=out_weight, expert_input=expert_input, expert_gain=expert_gain, routes=routes, route_weight=route_weight, gate_weight=gate_weight, up_weight=up_weight, down_weight=down_weight)


EPSILON = 1e-06
THETA = 10000.0

def normalize(entries, gain):
    wide = entries.astype(jnp.float32)
    factor = lax.rsqrt(lax.optimization_barrier(jnp.mean(wide * wide, axis=-1, keepdims=True)) + EPSILON)
    return wide * factor * gain.astype(jnp.float32)

def rotate(entries, positions):
    half = entries.shape[-1] // 2
    freqs = THETA ** (-jnp.arange(half, dtype=jnp.float32) / half)
    angle = positions.astype(jnp.float32)[:, None, None] * freqs[None, None, :]
    cosine = jnp.cos(angle)
    sine = jnp.sin(angle)
    first = entries[..., :half].astype(jnp.float32)
    second = entries[..., half:].astype(jnp.float32)
    turned = jnp.concatenate([first * cosine - second * sine, first * sine + second * cosine], axis=-1)
    return turned.astype(jnp.bfloat16)

def rounded(entries):
    return lax.optimization_barrier(entries.astype(jnp.bfloat16)).astype(jnp.float32)

def reference(query_plain, query_rotary, latent_input, rotary_key, key_weight, value_weight, latent_gain, head_gain, out_weight, expert_input, expert_gain, routes, route_weight, gate_weight, up_weight, down_weight):
    positions = jnp.arange(TOKENS_A, dtype=jnp.int32)
    latent = normalize(latent_input, latent_gain).astype(jnp.bfloat16)
    key_rotated = rotate(rotary_key.reshape(TOKENS_A, 1, ROTARY_DIM), positions).reshape(TOKENS_A, ROTARY_DIM)
    query_rotated = rotate(query_rotary.reshape(TOKENS_A, HEADS, ROTARY_DIM), positions)
    keys = jnp.dot(latent, key_weight, preferred_element_type=jnp.float32).astype(jnp.bfloat16)
    values = jnp.dot(latent, value_weight, preferred_element_type=jnp.float32).astype(jnp.bfloat16)
    keys_wide = keys.astype(jnp.float32).reshape(TOKENS_A, HEADS, PLAIN_DIM)
    values_wide = values.astype(jnp.float32).reshape(TOKENS_A, HEADS, VALUE_DIM)
    rotated_wide = key_rotated.astype(jnp.float32)
    queries = query_plain.reshape(TOKENS_A, HEADS, PLAIN_DIM)
    factor = (PLAIN_DIM + ROTARY_DIM) ** (-0.5)

    def attend(block):
        start = (block * TOK_A).astype(jnp.int32)
        query_block = lax.dynamic_slice_in_dim(queries, start, TOK_A, 0).astype(jnp.float32)
        turned_block = lax.dynamic_slice_in_dim(query_rotated, start, TOK_A, 0).astype(jnp.float32)
        scores = jnp.einsum('qhd,khd->hqk', query_block, keys_wide) + jnp.einsum('qhr,kr->hqk', turned_block, rotated_wide)
        scores = scores * factor
        query_positions = start + jnp.arange(TOK_A, dtype=jnp.int32)
        allowed = (positions[None, :] <= query_positions[:, None])[None]
        masked = jnp.where(allowed, scores, -jnp.inf)
        highest = lax.optimization_barrier(jnp.max(masked, axis=-1, keepdims=True))
        weights = jnp.where(allowed, jnp.exp(masked - highest), 0.0).astype(jnp.bfloat16)
        return jnp.einsum('hqk,khd->qhd', weights.astype(jnp.float32), values_wide)
    context = lax.map(attend, jnp.arange(N_EP, dtype=jnp.int32)).reshape(TOKENS_A, HEADS, VALUE_DIM)
    head_output = normalize(context, head_gain.reshape(HEADS, VALUE_DIM)).astype(jnp.bfloat16).reshape(TOKENS_A, HEADS * VALUE_DIM)
    group = HEADS * VALUE_DIM // N_TP
    attended = jnp.zeros((TOKENS_A, D), jnp.float32)
    for index in range(N_TP):
        attended = attended + rounded(jnp.dot(head_output[:, index * group:(index + 1) * group], out_weight[index * group:(index + 1) * group], preferred_element_type=jnp.float32))
    attended = attended.astype(jnp.bfloat16)
    normed = normalize(expert_input, expert_gain).astype(jnp.bfloat16)
    blocks = N_EP * N_TP
    chosen = routes.reshape(blocks, TOK_B * TOP)
    onehot = (chosen[:, :, None] == jnp.arange(EXPERTS, dtype=jnp.int32)[None, None, :]).astype(jnp.int32)
    ranks = lax.optimization_barrier(jnp.sum(jnp.cumsum(onehot, axis=1) * onehot, axis=2)) - 1
    sources = jnp.arange(blocks, dtype=jnp.int32)[:, None]
    slot_index = (chosen * (blocks * CAP) + sources * CAP + ranks).reshape(-1).astype(jnp.int32)
    buffer = jnp.zeros((EXPERTS * blocks * CAP, D), jnp.bfloat16).at[slot_index].set(jnp.repeat(normed, TOP, axis=0))
    buffer = buffer.reshape(EXPERTS, blocks * CAP, D)
    width = FF // N_TP

    def run_expert(inputs):
        expert_rows, gate_local, up_local, down_local = inputs
        gate = jnp.dot(expert_rows, gate_local, preferred_element_type=jnp.float32)
        upward = jnp.dot(expert_rows, up_local, preferred_element_type=jnp.float32)
        expert_hidden = (jax.nn.silu(gate) * upward).astype(jnp.bfloat16)
        result = jnp.zeros((expert_rows.shape[0], D), jnp.float32)
        for index in range(N_TP):
            result = result + rounded(jnp.dot(expert_hidden[:, index * width:(index + 1) * width], down_local[index * width:(index + 1) * width], preferred_element_type=jnp.float32))
        return result.astype(jnp.bfloat16)
    results = lax.map(run_expert, (buffer, gate_weight, up_weight, down_weight)).reshape(EXPERTS * blocks * CAP, D)
    picked = results[slot_index].astype(jnp.float32).reshape(TOKENS_B, TOP, D)
    expert_out = lax.optimization_barrier(jnp.sum(picked * route_weight.astype(jnp.float32)[:, :, None], axis=1)).astype(jnp.bfloat16)
    return (attended, expert_out)
```

```python
import jax
import jax.numpy as jnp
from jax import lax
from jax.experimental import pallas as pl
from jax.experimental.pallas import tpu as pltpu
from jax.sharding import Mesh
from jax.sharding import PartitionSpec as P

PLAIN_DIM = 64
ROTARY_DIM = 32
VALUE_DIM = 64
TOP = 2
LANES = 128
EP = ("ep_0", "ep_1")
GRP_EP = ("grp", "ep_0", "ep_1")
GRP_EP_TP = ("grp", "ep_0", "ep_1", "tp")

EPSILON = 1e-06
THETA = 10000.0
BF16 = jnp.bfloat16
F32 = jnp.float32


def normalize(entries, gain):
    wide = entries.astype(F32)
    factor = lax.rsqrt(jnp.mean(wide * wide, axis=-1, keepdims=True) + EPSILON)
    return wide * factor * gain.astype(F32)


def rotate(entries, positions):
    half = entries.shape[-1] // 2
    freqs = THETA ** (-jnp.arange(half, dtype=F32) / half)
    angle = positions.astype(F32)[:, None, None] * freqs[None, None, :]
    cosine = jnp.cos(angle)
    sine = jnp.sin(angle)
    first = entries[..., :half].astype(F32)
    second = entries[..., half:].astype(F32)
    turned = jnp.concatenate(
        [first * cosine - second * sine, first * sine + second * cosine], axis=-1
    )
    return turned.astype(BF16)


def ring(step):
    size = lax.axis_size("tp")
    return [(i, (i + step) % size) for i in range(size)]


def swapped(block):
    return lax.ppermute(block, "ep_1", [(0, 1), (1, 0)])


def carried(block, distance):
    n = lax.axis_size("ep_0")
    pairs = []
    for z in range(n):
        for core, step in ((0, distance), (1, -distance)):
            pairs.append((2 * z + core, 2 * ((z + step) % n) + core))
    return lax.ppermute(block, EP, pairs)


def ring_gather(own):
    cut = (own.shape[0] // 2 + 7) // 8 * 8
    from_left = lax.ppermute(own, "tp", ring(1))
    from_right = lax.ppermute(own, "tp", ring(-1))
    far_low = lax.ppermute(from_left[:cut], "tp", ring(1))
    far_high = lax.ppermute(from_right[cut:], "tp", ring(-1))
    return own, from_left, from_right, far_low, far_high


def ring_sum(own, to_left, to_right, far_low, far_high):
    cut = far_low.shape[0]
    low = lax.ppermute(far_low, "tp", ring(-1))
    high = lax.ppermute(far_high, "tp", ring(1))
    send_left = jnp.concatenate(
        [(to_left[:cut].astype(F32) + low.astype(F32)).astype(BF16), to_left[cut:]]
    )
    send_right = jnp.concatenate(
        [to_right[:cut], (to_right[cut:].astype(F32) + high.astype(F32)).astype(BF16)]
    )
    a = lax.ppermute(send_left, "tp", ring(-1))
    b = lax.ppermute(send_right, "tp", ring(1))
    return (own.astype(F32) + a.astype(F32) + b.astype(F32)).astype(BF16)


def attention_kernel(where_ref, latent_ref, head_ref, out_ref, score_ref, both_ref):
    span = 256
    ep, part = where_ref[0], where_ref[1]
    rows = head_ref.shape[1]
    quarter = where_ref[2]
    per = span // 64
    weights = head_ref[0, :, :LANES]
    query = head_ref[0, :, LANES:]
    factor = (PLAIN_DIM + ROTARY_DIM) ** (-0.5)
    count = ep // per + 1
    lane = lax.broadcasted_iota(jnp.int32, (span, LANES), 1)
    column = lax.broadcasted_iota(jnp.int32, (rows, span), 1)
    line = lax.broadcasted_iota(jnp.int32, (rows, span), 0)
    shift = column // 64 * quarter + column % 64

    def first(i, highest):
        begin = pl.multiple_of(i * span, span)
        both = jnp.dot(
            latent_ref[pl.ds(begin, span), : 2 * LANES], weights, preferred_element_type=F32
        ).astype(BF16)
        both_ref[pl.ds(begin, span), :] = both
        keys = jnp.where(lane < PLAIN_DIM, both, latent_ref[pl.ds(begin, span), 2 * LANES :])
        scores = (
            lax.dot_general(
                query, keys, (((1,), (1,)), ((), ())), preferred_element_type=F32
            )
            * factor
        )
        allowed = shift + (i * per * quarter + part * 64) <= line + ep * quarter
        scores = jnp.where(allowed, scores, -1e30)
        score_ref[:, pl.ds(begin, span)] = scores
        return jnp.maximum(highest, jnp.max(scores, axis=-1, keepdims=True))

    highest = lax.fori_loop(0, count, first, jnp.full((rows, 1), -1e30, F32))

    def second(i, total):
        begin = pl.multiple_of(i * span, span)
        scores = score_ref[:, pl.ds(begin, span)]
        kept = jnp.where(scores > -1e29, jnp.exp(scores - highest), 0.0).astype(BF16)
        return total + jnp.dot(kept, both_ref[pl.ds(begin, span), :], preferred_element_type=F32)

    total = lax.fori_loop(0, count, second, jnp.zeros((rows, LANES), F32))
    wide = lax.broadcasted_iota(jnp.int32, (rows, LANES), 1)
    out_ref[...] = jnp.where(wide < PLAIN_DIM, jnp.broadcast_to(highest, (rows, LANES)), total)


def attend(
    query_plain,
    query_rotary,
    latent_input,
    rotary_key,
    key_weight,
    value_weight,
    latent_gain,
    head_gain,
    out_weight,
):
    tokens = query_plain.shape[0]
    heads = key_weight.shape[1] // PLAIN_DIM
    count_tp = lax.axis_size("tp")
    part = tokens // count_tp
    ep = lax.axis_index(EP)
    core = lax.axis_index("ep_1")
    offset = ep * tokens
    positions = offset + jnp.arange(tokens, dtype=jnp.int32)
    begin = lax.axis_index("tp") * part
    own_latent = normalize(
        lax.dynamic_slice_in_dim(latent_input, begin, part, 0), latent_gain
    ).astype(BF16)
    own_rotated = rotate(
        lax.dynamic_slice_in_dim(rotary_key, begin, part, 0).reshape(part, 1, ROTARY_DIM),
        offset + begin + jnp.arange(part, dtype=jnp.int32),
    ).reshape(part, ROTARY_DIM)
    margin = LANES - PLAIN_DIM - ROTARY_DIM
    own = jnp.concatenate(
        [own_latent, jnp.pad(own_rotated, ((0, 0), (PLAIN_DIM, margin)))], axis=1
    )
    sibling = swapped(own)
    pair = jnp.where(
        core == 0, jnp.concatenate([own, sibling]), jnp.concatenate([sibling, own])
    )
    every = lax.all_gather(pair, "ep_0", axis=0, tiled=True)

    query_rotated = rotate(query_rotary.reshape(tokens, heads, ROTARY_DIM), positions)
    pieces = []
    for h in range(heads):
        cut = slice(h * PLAIN_DIM, (h + 1) * PLAIN_DIM)
        pieces += [
            key_weight[:, cut],
            value_weight[:, cut],
            query_plain[:, cut],
            query_rotated[:, h],
            jnp.zeros((tokens, margin), BF16),
        ]
    packed = jnp.concatenate(pieces, axis=1)
    width = packed.shape[1]
    blocks = out_weight.shape[1] // width
    lines = out_weight.shape[0]
    packed = jnp.concatenate(
        [packed] + [out_weight[:, i * width : (i + 1) * width] for i in range(blocks)]
    )
    shared = lax.all_gather(packed, "tp", axis=0)
    all_heads = heads * count_tp
    place = jnp.stack([ep, lax.axis_index("tp"), jnp.int32(tokens)]).astype(jnp.int32)
    partial = pl.pallas_call(
        attention_kernel,
        grid_spec=pltpu.PrefetchScalarGridSpec(
            num_scalar_prefetch=1,
            grid=(all_heads,),
            in_specs=[
                pl.BlockSpec(every.shape, lambda h, w: (0, 0)),
                pl.BlockSpec((1, tokens, 2 * LANES), lambda h, w: (h // heads, 0, h % heads)),
            ],
            out_specs=pl.BlockSpec((tokens, LANES), lambda h, w: (0, h)),
            scratch_shapes=[
                pltpu.VMEM((tokens, every.shape[0]), F32),
                pltpu.VMEM((every.shape[0], LANES), BF16),
            ],
        ),
        out_shape=jax.ShapeDtypeStruct((tokens, all_heads * LANES), F32),
        cost_estimate=pl.CostEstimate(
            flops=12_000_000_000, bytes_accessed=8_000_000, transcendentals=4_000_000
        ),
    )(place, every, shared)
    tiles = lax.all_to_all(partial.reshape(count_tp, part, -1), "tp", 0, 0, tiled=True)
    tiles = tiles.reshape(count_tp, part, all_heads, LANES)
    peaks = tiles[..., :1]
    sums = tiles[..., PLAIN_DIM:]
    context = jnp.sum(sums * jnp.exp(peaks - jnp.max(peaks, axis=0, keepdims=True)), axis=0)
    every_gain = lax.all_gather(head_gain, "tp", axis=0, tiled=True).reshape(all_heads, VALUE_DIM)
    head_output = normalize(context, every_gain).astype(BF16).reshape(part, -1)
    columns = []
    for i in range(blocks):
        total = jnp.zeros((part, width), F32)
        for g in range(count_tp):
            share = jnp.dot(
                head_output[:, g * lines : (g + 1) * lines],
                shared[g, tokens + i * lines : tokens + (i + 1) * lines],
                preferred_element_type=F32,
            )
            total = total + lax.reduce_precision(share, 8, 7)
        columns.append(total.astype(BF16))
    return jnp.concatenate(columns, axis=1)


def experts(expert_input, expert_gain, routes, route_weight, gate_weight, up_weight, down_weight):
    tokens, features = expert_input.shape
    count_ep = lax.axis_size(EP)
    n = lax.axis_size("ep_0")
    far = n // 2
    z, core = lax.axis_index("ep_0"), lax.axis_index("ep_1")
    sign = 1 - 2 * core
    cap = min(tokens, max(2, (9 * tokens + 4 * count_ep - 1) // (4 * count_ep)))
    groups = [[1]] + [[far - i, i + 1] for i in range(1, far // 2)]
    slot_step, slot_other, slot_bounds = [], [], [0]
    for k, group in enumerate(groups):
        listed = [(d, 0) for d in group for _ in (0, 1)]
        flips = [0, 1] * len(group)
        steps = [(d, True) for d in group for _ in (0, 1)]
        if k == 0:
            steps += [(far, True)] * 2 + [(0, True)] * 2
            flips += [0, 1, 0, 1]
        steps += [(d, False) for d in group for _ in (0, 1)]
        flips += [1, 0] * len(group)
        for (d, mine), flip in zip(steps, flips):
            slot_step += [d if mine else -d] * cap
            slot_other += [flip] * cap
        slot_bounds.append(len(slot_step))
    slot_rank = list(range(cap)) * (len(slot_step) // cap)
    slot_step = jnp.array(slot_step, jnp.int32)
    slot_other = jnp.array(slot_other, jnp.int32)
    slot_rank = jnp.array(slot_rank, jnp.int32)
    slot_expert = (z + sign * slot_step + 2 * n) % n * 2 + (core + slot_other) % 2
    slot_key = slot_expert * tokens + slot_rank

    ids = jnp.arange(count_ep, dtype=jnp.int32)
    named = routes[:, :, None] == ids
    onehot = jnp.sum(named.astype(BF16), axis=1)
    rows = jnp.arange(tokens, dtype=jnp.int32)
    earlier = jnp.dot(
        (rows[:, None] > rows[None, :]).astype(BF16), onehot, preferred_element_type=F32
    )
    ranks = jnp.sum(jnp.where(named, earlier[:, None, :], 0.0), axis=2).astype(jnp.int32)
    token_key = routes * tokens + ranks
    hits = token_key[:, :, None] == slot_key[None, None, :]
    selection = jnp.any(hits, axis=1).astype(BF16)
    shares = jnp.sum(jnp.where(hits, route_weight[:, :, None], 0.0), axis=1)
    coarse = lax.reduce_precision(shares, 8, 7)
    fine = (shares - coarse).astype(BF16)
    both_shares = jnp.concatenate([coarse.astype(BF16), fine], axis=0)
    normed = normalize(expert_input, expert_gain).astype(BF16)
    outgoing = lax.dot_general(
        selection, normed, (((0,), (0,)), ((), ())), preferred_element_type=F32
    ).astype(BF16)
    outgoing = outgoing.reshape(-1, features // LANES, LANES)

    gate_local = gate_weight[0]
    up_local = up_weight[0]
    down_local = down_weight[0]

    theirs, mine = [], []
    for k, group in enumerate(groups):
        block = outgoing[slot_bounds[k] : slot_bounds[k + 1]]
        size = 2 * cap * len(group)
        mine.append(block[: block.shape[0] - size])
        theirs.append(block[block.shape[0] - size :])
    half_way = carried(mine[0][2 * cap : 4 * cap], far)
    local = mine[0][4 * cap :]
    sibling = swapped(jnp.concatenate(theirs))
    at = 0
    arrived = []
    for k, group in enumerate(groups):
        blocks = []
        for j, d in enumerate(group):
            a = mine[k][2 * cap * j : 2 * cap * (j + 1)]
            b = sibling[at : at + 2 * cap]
            at += 2 * cap
            blocks.append(
                carried(jnp.concatenate([a[:cap], b[:cap], a[cap:], b[cap:]]), d)
            )
        arrived.append(blocks)

    combined = jnp.zeros((2 * tokens, features), F32)
    for k, group in enumerate(groups):
        keep = [b[: 2 * cap] for b in arrived[k]]
        send = [b[2 * cap :] for b in arrived[k]]
        if k == 0:
            keep += [half_way[:cap], local[:cap]]
            send += [half_way[cap:], local[cap:]]
        keep = jnp.concatenate(keep)
        size = keep.shape[0]
        block = jnp.concatenate([keep, swapped(jnp.concatenate(send))])
        block = block.reshape(2 * size, features)
        pieces = ring_gather(block)
        piece = jnp.concatenate(pieces, axis=0)
        gate = jnp.dot(piece, gate_local, preferred_element_type=F32)
        upward = jnp.dot(piece, up_local, preferred_element_type=F32)
        hidden = (jax.nn.silu(gate) * upward).astype(BF16)
        result = jnp.dot(hidden, down_local, preferred_element_type=F32).astype(BF16)
        ends, total = [], 0
        for p in pieces[:-1]:
            total += p.shape[0]
            ends.append(total)
        summed = ring_sum(*jnp.split(result, ends)).reshape(2 * size, features // LANES, LANES)
        keep = summed[:size]
        send = swapped(summed[size:])
        own_rows, sibling_rows = [], []
        for j, d in enumerate(group):
            cut = slice(2 * cap * j, 2 * cap * (j + 1))
            back = carried(jnp.concatenate([keep[cut], send[cut]]), -d)
            own_rows += [back[:cap], back[2 * cap : 3 * cap]]
            sibling_rows += [back[cap : 2 * cap], back[3 * cap :]]
        if k == 0:
            cut = slice(2 * cap, 3 * cap)
            own_rows.append(carried(jnp.concatenate([keep[cut], send[cut]]), far))
            own_rows += [keep[3 * cap :], send[3 * cap :]]
        rows_back = jnp.concatenate(own_rows + [swapped(jnp.concatenate(sibling_rows))])
        combined = combined + jnp.dot(
            both_shares[:, slot_bounds[k] : slot_bounds[k + 1]],
            rows_back.reshape(-1, features),
            preferred_element_type=F32,
        )
    return (combined[:tokens] + combined[tokens:]).astype(BF16)


def body(
    query_plain,
    query_rotary,
    latent_input,
    rotary_key,
    key_weight,
    value_weight,
    latent_gain,
    head_gain,
    out_weight,
    expert_input,
    expert_gain,
    routes,
    route_weight,
    gate_weight,
    up_weight,
    down_weight,
):
    attended = attend(
        query_plain,
        query_rotary,
        latent_input,
        rotary_key,
        key_weight,
        value_weight,
        latent_gain,
        head_gain,
        out_weight,
    )
    expert_out = experts(
        expert_input, expert_gain, routes, route_weight, gate_weight, up_weight, down_weight
    )
    return (attended, expert_out)


def solution(mesh):
    finer = Mesh(
        mesh.devices.reshape(mesh.shape["grp"], 16, 2, mesh.shape["tp"]),
        ("grp", "ep_0", "ep_1", "tp"),
    )
    in_specs = (
        P(GRP_EP, "tp"),
        P(GRP_EP, "tp"),
        P(GRP_EP, None),
        P(GRP_EP, None),
        P(None, "tp"),
        P(None, "tp"),
        P(),
        P("tp"),
        P("tp", None),
        P(GRP_EP_TP, None),
        P(),
        P(GRP_EP_TP, None),
        P(GRP_EP_TP, None),
        P(EP, None, "tp"),
        P(EP, None, "tp"),
        P(EP, "tp", None),
    )
    out_specs = (P(GRP_EP_TP, None), P(GRP_EP_TP, None))
    return jax.shard_map(body, mesh=finer, in_specs=in_specs, out_specs=out_specs, check_vma=False)
```

```python
import jax
import jax.numpy as jnp
from jax import lax
from jax.experimental import pallas as pl
from jax.experimental.pallas import tpu as pltpu
from jax.sharding import Mesh
from jax.sharding import PartitionSpec as P


PLAIN_DIM = 64
ROTARY_DIM = 32
VALUE_DIM = 64
TOP = 2
LANES = 128
EP = ("ep_0", "ep_1")
GRP_EP = ("grp", "ep_0", "ep_1")
GRP_EP_TP = ("grp", "ep_0", "ep_1", "tp")

CHUNKS = 2
EPSILON = 1e-06
THETA = 10000.0
BF16 = jnp.bfloat16
F32 = jnp.float32


def normalize(entries, gain):
    wide = entries.astype(F32)
    factor = lax.rsqrt(jnp.mean(wide * wide, axis=-1, keepdims=True) + EPSILON)
    return wide * factor * gain.astype(F32)


def rotate(entries, positions):
    half = entries.shape[-1] // 2
    freqs = THETA ** (-jnp.arange(half, dtype=F32) / half)
    angle = positions.astype(F32)[:, None, None] * freqs[None, None, :]
    cosine = jnp.cos(angle)
    sine = jnp.sin(angle)
    first = entries[..., :half].astype(F32)
    second = entries[..., half:].astype(F32)
    turned = jnp.concatenate(
        [first * cosine - second * sine, first * sine + second * cosine], axis=-1
    )
    return turned.astype(BF16)


def ring(step):
    size = lax.axis_size("tp")
    return [(i, (i + step) % size) for i in range(size)]


def swapped(block):
    return lax.ppermute(block, "ep_1", [(0, 1), (1, 0)])


def ring_gather(own):
    cut = (own.shape[0] // 2 + 7) // 8 * 8
    from_left = lax.ppermute(own, "tp", ring(1))
    from_right = lax.ppermute(own, "tp", ring(-1))
    far_low = lax.ppermute(from_left[:cut], "tp", ring(1))
    far_high = lax.ppermute(from_right[cut:], "tp", ring(-1))
    return own, from_left, from_right, far_low, far_high


def ring_sum(own, to_left, to_right, far_low, far_high):
    cut = far_low.shape[0]
    low = lax.ppermute(far_low, "tp", ring(-1))
    high = lax.ppermute(far_high, "tp", ring(1))
    send_left = jnp.concatenate(
        [(to_left[:cut].astype(F32) + low.astype(F32)).astype(BF16), to_left[cut:]]
    )
    send_right = jnp.concatenate(
        [to_right[:cut], (to_right[cut:].astype(F32) + high.astype(F32)).astype(BF16)]
    )
    a = lax.ppermute(send_left, "tp", ring(-1))
    b = lax.ppermute(send_right, "tp", ring(1))
    return (own.astype(F32) + a.astype(F32) + b.astype(F32)).astype(BF16)


def attention_kernel(where_ref, latent_ref, head_ref, out_ref, score_ref, both_ref):
    span = 512
    ep, part, quarter = where_ref[0], where_ref[1], where_ref[2]
    rows = head_ref.shape[1]
    per = span // 64
    weights = head_ref[0, :, :LANES]
    query = head_ref[0, :, LANES:]
    factor = (PLAIN_DIM + ROTARY_DIM) ** (-0.5) * 1.4426950408889634
    last = ep // per
    lane = lax.broadcasted_iota(jnp.int32, (span, LANES), 1)

    def scored(i):
        begin = pl.multiple_of(i * span, span)
        both = jnp.dot(
            latent_ref[pl.ds(begin, span), : 2 * LANES], weights, preferred_element_type=F32
        ).astype(BF16)
        both_ref[pl.ds(begin, span), :] = both
        keys = jnp.where(lane < PLAIN_DIM, both, latent_ref[pl.ds(begin, span), 2 * LANES :])
        return (
            lax.dot_general(query, keys, (((1,), (1,)), ((), ())), preferred_element_type=F32)
            * factor
        )

    def first(i, highest):
        scores = scored(i)
        score_ref[:, pl.ds(pl.multiple_of(i * span, span), span)] = scores
        return jnp.maximum(highest, jnp.max(scores, axis=-1, keepdims=True))

    highest = lax.fori_loop(0, last, first, jnp.full((rows, 1), -1e30, F32))
    scores = scored(last)
    column = lax.broadcasted_iota(jnp.int32, (rows, span), 1)
    line = lax.broadcasted_iota(jnp.int32, (rows, span), 0)
    key_place = (column // 64 + last * per) * quarter + part * 64 + column % 64
    scores = jnp.where(key_place <= line + ep * quarter, scores, -1e30)
    score_ref[:, pl.ds(pl.multiple_of(last * span, span), span)] = scores
    highest = jnp.maximum(highest, jnp.max(scores, axis=-1, keepdims=True))

    def second(i, total):
        begin = pl.multiple_of(i * span, span)
        kept = jnp.exp2(score_ref[:, pl.ds(begin, span)] - highest).astype(BF16)
        return total + jnp.dot(kept, both_ref[pl.ds(begin, span), :], preferred_element_type=F32)

    total = lax.fori_loop(0, last + 1, second, jnp.zeros((rows, LANES), F32))
    wide = lax.broadcasted_iota(jnp.int32, (rows, LANES), 1)
    out_ref[...] = jnp.where(wide < PLAIN_DIM, jnp.broadcast_to(highest, (rows, LANES)), total)


def finish_kernel(where_ref, tiles_ref, shared_ref, out_ref, total_ref):
    p = pl.program_id(0)
    rows = tiles_ref.shape[1]
    lines = LANES
    start = shared_ref.shape[1] - 16
    width = shared_ref.shape[2]
    blocks = out_ref.shape[1] // width
    lane = lax.broadcasted_iota(jnp.int32, (rows, LANES), 1)
    outputs = []
    for h in range(2):
        block = tiles_ref[:, :, h * LANES : (h + 1) * LANES]
        peaks = [pltpu.roll(block[i], PLAIN_DIM, 1) for i in range(block.shape[0])]
        top = peaks[0]
        for other in peaks[1:]:
            top = jnp.maximum(top, other)
        context = jnp.zeros((rows, LANES), F32)
        for i, peak in enumerate(peaks):
            context = context + block[i] * jnp.exp2(peak - top)
        context = jnp.where(lane < PLAIN_DIM, 0.0, context)
        mean = jnp.sum(context * context, axis=-1, keepdims=True) / VALUE_DIM
        gain = shared_ref[0, start : start + 16, h * LANES : (h + 1) * LANES].astype(F32)[:1]
        outputs.append(context * lax.rsqrt(mean + EPSILON) * gain)
    head_output = jnp.where(
        lane < PLAIN_DIM, pltpu.roll(outputs[0], PLAIN_DIM, 1), outputs[1]
    ).astype(BF16)
    for i in range(blocks):
        at = start - (blocks - i) * lines
        share = jnp.dot(
            head_output, shared_ref[0, at : at + lines, :], preferred_element_type=F32
        ).astype(BF16).astype(F32)
        cut = slice(i * width, (i + 1) * width)

        @pl.when(p == 0)
        def _():
            total_ref[:, cut] = share

        @pl.when(p > 0)
        def _():
            total_ref[:, cut] = total_ref[:, cut] + share

    @pl.when(p == pl.num_programs(0) - 1)
    def _():
        out_ref[...] = total_ref[...].astype(BF16)


def route_kernel(input_ref, gain_ref, route_ref, weight_ref, key_ref, rows_ref, shares_ref):
    tokens = input_ref.shape[0]
    wide = input_ref[...].astype(F32)
    factor = lax.rsqrt(jnp.mean(wide * wide, axis=-1, keepdims=True) + EPSILON)
    normed = (wide * factor * gain_ref[...].astype(F32)).astype(BF16)
    lane = lax.broadcasted_iota(jnp.int32, (tokens, LANES), 1)
    named = [route_ref[:, k : k + 1] == lane for k in range(TOP)]
    onehot = jnp.where(named[0] | named[1], 1.0, 0.0).astype(BF16)
    line = lax.broadcasted_iota(jnp.int32, (tokens, tokens), 0)
    column = lax.broadcasted_iota(jnp.int32, (tokens, tokens), 1)
    before = jnp.where(line > column, 1.0, 0.0).astype(BF16)
    earlier = jnp.dot(before, onehot, preferred_element_type=F32)
    slots = key_ref.shape[1]
    slot_key = jnp.broadcast_to(key_ref[...], (tokens, slots))
    selection = jnp.zeros((tokens, slots), F32)
    shares = jnp.zeros((tokens, slots), F32)
    for k in range(TOP):
        rank = jnp.sum(jnp.where(named[k], earlier, 0.0), axis=1, keepdims=True)
        key = route_ref[:, k : k + 1] * tokens + rank.astype(jnp.int32)
        hit = key == slot_key
        selection = selection + jnp.where(hit, 1.0, 0.0)
        shares = shares + jnp.where(hit, weight_ref[:, k : k + 1], 0.0)
    coarse = shares.astype(BF16)
    shares_ref[:tokens] = coarse
    shares_ref[tokens:] = (shares - coarse.astype(F32)).astype(BF16)
    rows_ref[...] = lax.dot_general(
        selection.astype(BF16), normed, (((0,), (0,)), ((), ())), preferred_element_type=F32
    ).astype(BF16)


def prepare(
    query_plain,
    query_rotary,
    latent_input,
    rotary_key,
    key_weight,
    value_weight,
    latent_gain,
    head_gain,
    out_weight,
):
    tokens = query_plain.shape[0]
    heads = key_weight.shape[1] // PLAIN_DIM
    count_tp = lax.axis_size("tp")
    part = tokens // count_tp
    ep = lax.axis_index(EP)
    core = lax.axis_index("ep_1")
    offset = ep * tokens
    positions = offset + jnp.arange(tokens, dtype=jnp.int32)
    begin = lax.axis_index("tp") * part
    own_latent = normalize(
        lax.dynamic_slice_in_dim(latent_input, begin, part, 0), latent_gain
    ).astype(BF16)
    own_rotated = rotate(
        lax.dynamic_slice_in_dim(rotary_key, begin, part, 0).reshape(part, 1, ROTARY_DIM),
        offset + begin + jnp.arange(part, dtype=jnp.int32),
    ).reshape(part, ROTARY_DIM)
    margin = LANES - PLAIN_DIM - ROTARY_DIM
    own = jnp.concatenate(
        [own_latent, jnp.pad(own_rotated, ((0, 0), (PLAIN_DIM, margin)))], axis=1
    )
    sibling = swapped(own)
    pair = jnp.where(
        core == 0, jnp.concatenate([own, sibling]), jnp.concatenate([sibling, own])
    )
    every = lax.all_gather(pair, "ep_0", axis=0, tiled=True)

    query_rotated = rotate(query_rotary.reshape(tokens, heads, ROTARY_DIM), positions)
    pieces = []
    for h in range(heads):
        cut = slice(h * PLAIN_DIM, (h + 1) * PLAIN_DIM)
        pieces += [
            key_weight[:, cut],
            value_weight[:, cut],
            query_plain[:, cut],
            query_rotated[:, h],
            jnp.zeros((tokens, margin), BF16),
        ]
    packed = jnp.concatenate(pieces, axis=1)
    width = packed.shape[1]
    blocks = out_weight.shape[1] // width
    gains = jnp.zeros((16, width), BF16)
    for h in range(heads):
        cut = slice(h * PLAIN_DIM, (h + 1) * PLAIN_DIM)
        place = slice(h * LANES + PLAIN_DIM, (h + 1) * LANES)
        gains = gains.at[:, place].set(jnp.broadcast_to(head_gain[cut], (16, PLAIN_DIM)))
    packed = jnp.concatenate(
        [packed] + [out_weight[:, i * width : (i + 1) * width] for i in range(blocks)] + [gains]
    )
    shared = jnp.concatenate(ring_gather(packed)).reshape(count_tp, *packed.shape)
    return every, shared


def attend(every, shared, tokens, heads):
    count_tp = shared.shape[0]
    width = shared.shape[2]
    part = tokens // count_tp
    blocks = (shared.shape[1] - tokens - 16) // LANES
    ep = lax.axis_index(EP)
    all_heads = heads * count_tp
    me = lax.axis_index("tp")
    order = [me] + [(me + i) % count_tp for i in (-1, 1, 2)]
    place = jnp.stack([ep, me, jnp.int32(tokens)] + order).astype(jnp.int32)
    attention = pl.pallas_call(
        attention_kernel,
        grid_spec=pltpu.PrefetchScalarGridSpec(
            num_scalar_prefetch=1,
            grid=(all_heads,),
            in_specs=[
                pl.BlockSpec(every.shape, lambda h, w: (0, 0)),
                pl.BlockSpec((1, tokens, 2 * LANES), lambda h, w: (h // heads, 0, h % heads)),
            ],
            out_specs=pl.BlockSpec(
                (tokens, LANES), lambda h, w: (0, w[3 + h // heads] * heads + h % heads)
            ),
            scratch_shapes=[
                pltpu.VMEM((tokens, every.shape[0]), F32),
                pltpu.VMEM((every.shape[0], LANES), BF16),
            ],
        ),
        out_shape=jax.ShapeDtypeStruct((tokens, all_heads * LANES), F32),
        cost_estimate=pl.CostEstimate(
            flops=12_000_000_000, bytes_accessed=8_000_000, transcendentals=4_000_000
        ),
    )
    partial = attention(place, every, shared)
    tiles = partial.reshape(count_tp, part, -1)

    def block(step):
        return lax.dynamic_slice_in_dim(tiles, (me + step) % count_tp, 1, 0)

    sent = [lax.ppermute(block(i), "tp", ring(i)) for i in (1, -1, 2)]
    tiles = jnp.concatenate([block(0)] + sent)
    return pl.pallas_call(
        finish_kernel,
        grid_spec=pltpu.PrefetchScalarGridSpec(
            num_scalar_prefetch=1,
            grid=(count_tp,),
            in_specs=[
                pl.BlockSpec((count_tp, part, heads * LANES), lambda p, w: (0, 0, w[3 + p])),
                pl.BlockSpec((1, *shared.shape[1:]), lambda p, w: (p, 0, 0)),
            ],
            out_specs=pl.BlockSpec((part, blocks * width), lambda p, w: (0, 0)),
            scratch_shapes=[pltpu.VMEM((part, blocks * width), F32)],
        ),
        out_shape=jax.ShapeDtypeStruct((part, blocks * width), BF16),
        cost_estimate=pl.CostEstimate(
            flops=200_000_000, bytes_accessed=4_000_000, transcendentals=300_000
        ),
    )(place, tiles, shared)


def route(expert_input, expert_gain, routes, route_weight):
    tokens, features = expert_input.shape
    count_ep = lax.axis_size(EP)
    cap = min(tokens, max(2, (9 * tokens + 4 * count_ep - 1) // (4 * count_ep)))
    slots = jnp.arange(count_ep * cap, dtype=jnp.int32)
    slot_key = slots // cap * tokens + slots % cap
    return pl.pallas_call(
        route_kernel,
        out_shape=(
            jax.ShapeDtypeStruct((count_ep * cap, features), BF16),
            jax.ShapeDtypeStruct((2 * tokens, count_ep * cap), BF16),
        ),
        cost_estimate=pl.CostEstimate(
            flops=200_000_000, bytes_accessed=2_000_000, transcendentals=0
        ),
    )(expert_input, expert_gain[None], routes, route_weight, slot_key[None])


def exchanged(rows):
    count, features = rows.shape
    size = lax.axis_size(EP)
    tiles = rows.reshape(size, count // size, features // LANES, LANES)
    return lax.all_to_all(tiles, EP, 0, 0, tiled=True).reshape(count, features)


def experts(arrived, gate_weight, up_weight, down_weight):
    gate_local, up_local, down_local = gate_weight[0], up_weight[0], down_weight[0]
    count = arrived.shape[0] // CHUNKS
    gathered = [ring_gather(arrived[c * count : (c + 1) * count]) for c in range(CHUNKS)]
    sums = []
    for pieces in gathered:
        piece = jnp.concatenate(pieces, axis=0)
        gate = jnp.dot(piece, gate_local, preferred_element_type=F32)
        upward = jnp.dot(piece, up_local, preferred_element_type=F32)
        hidden = (jax.nn.silu(gate) * upward).astype(BF16)
        result = jnp.dot(hidden, down_local, preferred_element_type=F32).astype(BF16)
        ends, total = [], 0
        for p in pieces[:-1]:
            total += p.shape[0]
            ends.append(total)
        sums.append(ring_sum(*jnp.split(result, ends)))
    return jnp.concatenate(sums)


def body(
    query_plain,
    query_rotary,
    latent_input,
    rotary_key,
    key_weight,
    value_weight,
    latent_gain,
    head_gain,
    out_weight,
    expert_input,
    expert_gain,
    routes,
    route_weight,
    gate_weight,
    up_weight,
    down_weight,
):
    tokens = query_plain.shape[0]
    heads = key_weight.shape[1] // PLAIN_DIM
    outgoing, shares = route(expert_input, expert_gain, routes, route_weight)
    outgoing, query_plain, query_rotary, latent_input, rotary_key = lax.optimization_barrier(
        (outgoing, query_plain, query_rotary, latent_input, rotary_key)
    )
    arrived = exchanged(outgoing)
    every, shared = prepare(
        query_plain,
        query_rotary,
        latent_input,
        rotary_key,
        key_weight,
        value_weight,
        latent_gain,
        head_gain,
        out_weight,
    )
    sums = experts(arrived, gate_weight, up_weight, down_weight)
    sums, every, shared = lax.optimization_barrier((sums, every, shared))
    returned = exchanged(sums)
    attended = attend(every, shared, tokens, heads)
    combined = jnp.dot(shares, returned, preferred_element_type=F32)
    rows = expert_input.shape[0]
    return (attended, (combined[:rows] + combined[rows:]).astype(BF16))


def solution(mesh):
    finer = Mesh(
        mesh.devices.reshape(mesh.shape["grp"], 16, 2, mesh.shape["tp"]),
        ("grp", "ep_0", "ep_1", "tp"),
    )
    in_specs = (
        P(GRP_EP, "tp"),
        P(GRP_EP, "tp"),
        P(GRP_EP, None),
        P(GRP_EP, None),
        P(None, "tp"),
        P(None, "tp"),
        P(),
        P("tp"),
        P("tp", None),
        P(GRP_EP_TP, None),
        P(),
        P(GRP_EP_TP, None),
        P(GRP_EP_TP, None),
        P(EP, None, "tp"),
        P(EP, None, "tp"),
        P(EP, "tp", None),
    )
    out_specs = (P(GRP_EP_TP, None), P(GRP_EP_TP, None))
    return jax.shard_map(body, mesh=finer, in_specs=in_specs, out_specs=out_specs, check_vma=False)
```

```python
from functools import partial

import jax
import jax.numpy as jnp
from jax import lax
from jax.experimental import pallas as pl
from jax.experimental.pallas import tpu as pltpu
from jax.sharding import Mesh
from jax.sharding import PartitionSpec as P


PLAIN_DIM = 64
ROTARY_DIM = 32
VALUE_DIM = 64
TOP = 2
LANES = 128
EP = ("ep_0", "ep_1")
GRP_EP = ("grp", "ep_0", "ep_1")
GRP_EP_TP = ("grp", "ep_0", "ep_1", "tp")

CHUNKS = 2
EPSILON = 1e-06
THETA = 10000.0
BF16 = jnp.bfloat16
F32 = jnp.float32


def normalize(entries, gain):
    wide = entries.astype(F32)
    factor = lax.rsqrt(jnp.mean(wide * wide, axis=-1, keepdims=True) + EPSILON)
    return wide * factor * gain.astype(F32)


def rotate(entries, positions):
    half = entries.shape[-1] // 2
    freqs = THETA ** (-jnp.arange(half, dtype=F32) / half)
    angle = positions.astype(F32)[:, None, None] * freqs[None, None, :]
    cosine = jnp.cos(angle)
    sine = jnp.sin(angle)
    first = entries[..., :half].astype(F32)
    second = entries[..., half:].astype(F32)
    turned = jnp.concatenate(
        [first * cosine - second * sine, first * sine + second * cosine], axis=-1
    )
    return turned.astype(BF16)


def ring(step):
    size = lax.axis_size("tp")
    return [(i, (i + step) % size) for i in range(size)]


def ring_gather(own):
    cut = (own.shape[0] // 2 + 7) // 8 * 8
    from_left = lax.ppermute(own, "tp", ring(1))
    from_right = lax.ppermute(own, "tp", ring(-1))
    far_low = lax.ppermute(from_left[:cut], "tp", ring(1))
    far_high = lax.ppermute(from_right[cut:], "tp", ring(-1))
    return own, from_left, from_right, far_low, far_high


def ring_sum(own, to_left, to_right, far_low, far_high):
    cut = far_low.shape[0]
    low = lax.ppermute(far_low, "tp", ring(-1))
    high = lax.ppermute(far_high, "tp", ring(1))
    send_left = jnp.concatenate(
        [(to_left[:cut].astype(F32) + low.astype(F32)).astype(BF16), to_left[cut:]]
    )
    send_right = jnp.concatenate(
        [to_right[:cut], (to_right[cut:].astype(F32) + high.astype(F32)).astype(BF16)]
    )
    a = lax.ppermute(send_left, "tp", ring(-1))
    b = lax.ppermute(send_right, "tp", ring(1))
    return (own.astype(F32) + a.astype(F32) + b.astype(F32)).astype(BF16)


def attention_kernel(where_ref, latent_ref, head_ref, out_ref, score_ref, both_ref):
    span = 512
    ep, part, quarter = where_ref[0], where_ref[1], where_ref[2]
    rows = head_ref.shape[1]
    per = span // 64
    weights = head_ref[0, :, :LANES]
    query = head_ref[0, :, LANES:]
    factor = (PLAIN_DIM + ROTARY_DIM) ** (-0.5) * 1.4426950408889634
    last = ep // per
    lane = lax.broadcasted_iota(jnp.int32, (span, LANES), 1)

    def scored(i):
        begin = pl.multiple_of(i * span, span)
        both = jnp.dot(
            latent_ref[pl.ds(begin, span), : 2 * LANES], weights, preferred_element_type=F32
        ).astype(BF16)
        both_ref[pl.ds(begin, span), :] = both
        keys = jnp.where(lane < PLAIN_DIM, both, latent_ref[pl.ds(begin, span), 2 * LANES :])
        return (
            lax.dot_general(query, keys, (((1,), (1,)), ((), ())), preferred_element_type=F32)
            * factor
        )

    def first(i, highest):
        scores = scored(i)
        score_ref[:, pl.ds(pl.multiple_of(i * span, span), span)] = scores
        return jnp.maximum(highest, jnp.max(scores, axis=-1, keepdims=True))

    highest = lax.fori_loop(0, last, first, jnp.full((rows, 1), -1e30, F32))
    scores = scored(last)
    column = lax.broadcasted_iota(jnp.int32, (rows, span), 1)
    line = lax.broadcasted_iota(jnp.int32, (rows, span), 0)
    key_place = (column // 64 + last * per) * quarter + part * 64 + column % 64
    scores = jnp.where(key_place <= line + ep * quarter, scores, -1e30)
    score_ref[:, pl.ds(pl.multiple_of(last * span, span), span)] = scores
    highest = jnp.maximum(highest, jnp.max(scores, axis=-1, keepdims=True))

    def second(i, total):
        begin = pl.multiple_of(i * span, span)
        kept = jnp.exp2(score_ref[:, pl.ds(begin, span)] - highest).astype(BF16)
        return total + jnp.dot(kept, both_ref[pl.ds(begin, span), :], preferred_element_type=F32)

    total = lax.fori_loop(0, last + 1, second, jnp.zeros((rows, LANES), F32))
    wide = lax.broadcasted_iota(jnp.int32, (rows, LANES), 1)
    out_ref[...] = jnp.where(wide < PLAIN_DIM, jnp.broadcast_to(highest, (rows, LANES)), total)


def finish_kernel(where_ref, tiles_ref, shared_ref, out_ref, total_ref):
    p = pl.program_id(0)
    rows = tiles_ref.shape[1]
    lines = LANES
    start = shared_ref.shape[1] - 16
    width = shared_ref.shape[2]
    blocks = out_ref.shape[1] // width
    lane = lax.broadcasted_iota(jnp.int32, (rows, LANES), 1)
    outputs = []
    for h in range(2):
        block = tiles_ref[:, :, h * LANES : (h + 1) * LANES]
        peaks = [pltpu.roll(block[i], PLAIN_DIM, 1) for i in range(block.shape[0])]
        top = peaks[0]
        for other in peaks[1:]:
            top = jnp.maximum(top, other)
        context = jnp.zeros((rows, LANES), F32)
        for i, peak in enumerate(peaks):
            context = context + block[i] * jnp.exp2(peak - top)
        context = jnp.where(lane < PLAIN_DIM, 0.0, context)
        mean = jnp.sum(context * context, axis=-1, keepdims=True) / VALUE_DIM
        gain = shared_ref[0, start : start + 16, h * LANES : (h + 1) * LANES].astype(F32)[:1]
        outputs.append(context * lax.rsqrt(mean + EPSILON) * gain)
    head_output = jnp.where(
        lane < PLAIN_DIM, pltpu.roll(outputs[0], PLAIN_DIM, 1), outputs[1]
    ).astype(BF16)
    for i in range(blocks):
        at = start - (blocks - i) * lines
        share = jnp.dot(
            head_output, shared_ref[0, at : at + lines, :], preferred_element_type=F32
        ).astype(BF16).astype(F32)
        cut = slice(i * width, (i + 1) * width)

        @pl.when(p == 0)
        def _():
            total_ref[:, cut] = share

        @pl.when(p > 0)
        def _():
            total_ref[:, cut] = total_ref[:, cut] + share

    @pl.when(p == pl.num_programs(0) - 1)
    def _():
        out_ref[...] = total_ref[...].astype(BF16)


def route_kernel(cap, input_ref, gain_ref, route_ref, weight_ref, rows_ref, shares_ref):
    tokens = input_ref.shape[0]
    wide = input_ref[...].astype(F32)
    factor = lax.rsqrt(jnp.mean(wide * wide, axis=-1, keepdims=True) + EPSILON)
    normed = (wide * factor * gain_ref[...].astype(F32)).astype(BF16)
    slots = rows_ref.shape[0]
    ids = lax.broadcasted_iota(jnp.int32, (slots // cap, tokens), 0)
    named = [ids == route_ref[k : k + 1, :] for k in range(TOP)]
    onehot = jnp.where(named[0] | named[1], 1.0, 0.0).astype(BF16)
    line = lax.broadcasted_iota(jnp.int32, (tokens, tokens), 0)
    column = lax.broadcasted_iota(jnp.int32, (tokens, tokens), 1)
    before = jnp.where(line < column, 1.0, 0.0).astype(BF16)
    earlier = jnp.dot(onehot, before, preferred_element_type=F32)
    slot = lax.broadcasted_iota(jnp.int32, (slots, tokens), 0)
    selection = jnp.zeros((slots, tokens), F32)
    shares = jnp.zeros((slots, tokens), F32)
    for k in range(TOP):
        rank = jnp.sum(jnp.where(named[k], earlier, 0.0), axis=0, keepdims=True)
        hit = slot == route_ref[k : k + 1, :] * cap + rank.astype(jnp.int32)
        selection = selection + jnp.where(hit, 1.0, 0.0)
        shares = shares + jnp.where(hit, weight_ref[k : k + 1, :], 0.0)
    coarse = shares.astype(BF16)
    shares_ref[:, :tokens] = coarse
    shares_ref[:, tokens:] = (shares - coarse.astype(F32)).astype(BF16)
    rows_ref[...] = jnp.dot(
        selection.astype(BF16), normed, preferred_element_type=F32
    ).astype(BF16)


def prepare(
    query_plain,
    query_rotary,
    latent_input,
    rotary_key,
    key_weight,
    value_weight,
    latent_gain,
    head_gain,
    out_weight,
):
    tokens = query_plain.shape[0]
    heads = key_weight.shape[1] // PLAIN_DIM
    count_tp = lax.axis_size("tp")
    part = tokens // count_tp
    ep = lax.axis_index(EP)
    offset = ep * tokens
    positions = offset + jnp.arange(tokens, dtype=jnp.int32)
    begin = lax.axis_index("tp") * part
    own_latent = normalize(
        lax.dynamic_slice_in_dim(latent_input, begin, part, 0), latent_gain
    ).astype(BF16)
    own_rotated = rotate(
        lax.dynamic_slice_in_dim(rotary_key, begin, part, 0).reshape(part, 1, ROTARY_DIM),
        offset + begin + jnp.arange(part, dtype=jnp.int32),
    ).reshape(part, ROTARY_DIM)
    margin = LANES - PLAIN_DIM - ROTARY_DIM
    own = jnp.concatenate(
        [own_latent, jnp.pad(own_rotated, ((0, 0), (PLAIN_DIM, margin)))], axis=1
    )
    count_ep = lax.axis_size(EP)
    copies = jnp.broadcast_to(own[None], (count_ep, *own.shape))
    every = lax.all_to_all(copies, EP, 0, 0, tiled=True).reshape(-1, own.shape[1])

    query_rotated = rotate(query_rotary.reshape(tokens, heads, ROTARY_DIM), positions)
    pieces = []
    for h in range(heads):
        cut = slice(h * PLAIN_DIM, (h + 1) * PLAIN_DIM)
        pieces += [
            key_weight[:, cut],
            value_weight[:, cut],
            query_plain[:, cut],
            query_rotated[:, h],
            jnp.zeros((tokens, margin), BF16),
        ]
    packed = jnp.concatenate(pieces, axis=1)
    width = packed.shape[1]
    blocks = out_weight.shape[1] // width
    gains = jnp.zeros((16, width), BF16)
    for h in range(heads):
        cut = slice(h * PLAIN_DIM, (h + 1) * PLAIN_DIM)
        place = slice(h * LANES + PLAIN_DIM, (h + 1) * LANES)
        gains = gains.at[:, place].set(jnp.broadcast_to(head_gain[cut], (16, PLAIN_DIM)))
    packed = jnp.concatenate(
        [packed] + [out_weight[:, i * width : (i + 1) * width] for i in range(blocks)] + [gains]
    )
    shared = jnp.concatenate(ring_gather(packed)).reshape(count_tp, *packed.shape)
    return every, shared


def attend(every, shared, tokens, heads):
    count_tp = shared.shape[0]
    width = shared.shape[2]
    part = tokens // count_tp
    blocks = (shared.shape[1] - tokens - 16) // LANES
    ep = lax.axis_index(EP)
    all_heads = heads * count_tp
    me = lax.axis_index("tp")
    order = [me] + [(me + i) % count_tp for i in (-1, 1, 2)]
    place = jnp.stack([ep, me, jnp.int32(tokens)] + order).astype(jnp.int32)
    attention = pl.pallas_call(
        attention_kernel,
        grid_spec=pltpu.PrefetchScalarGridSpec(
            num_scalar_prefetch=1,
            grid=(all_heads,),
            in_specs=[
                pl.BlockSpec(every.shape, lambda h, w: (0, 0)),
                pl.BlockSpec((1, tokens, 2 * LANES), lambda h, w: (h // heads, 0, h % heads)),
            ],
            out_specs=pl.BlockSpec(
                (tokens, LANES), lambda h, w: (0, w[3 + h // heads] * heads + h % heads)
            ),
            scratch_shapes=[
                pltpu.VMEM((tokens, every.shape[0]), F32),
                pltpu.VMEM((every.shape[0], LANES), BF16),
            ],
        ),
        out_shape=jax.ShapeDtypeStruct((tokens, all_heads * LANES), F32),
        cost_estimate=pl.CostEstimate(
            flops=12_000_000_000, bytes_accessed=8_000_000, transcendentals=4_000_000
        ),
    )
    sums = attention(place, every, shared)
    tiles = sums.reshape(count_tp, part, -1)

    def block(step):
        return lax.dynamic_slice_in_dim(tiles, (me + step) % count_tp, 1, 0)

    sent = [lax.ppermute(block(i), "tp", ring(i)) for i in (1, -1, 2)]
    tiles = jnp.concatenate([block(0)] + sent)
    return pl.pallas_call(
        finish_kernel,
        grid_spec=pltpu.PrefetchScalarGridSpec(
            num_scalar_prefetch=1,
            grid=(count_tp,),
            in_specs=[
                pl.BlockSpec((count_tp, part, heads * LANES), lambda p, w: (0, 0, w[3 + p])),
                pl.BlockSpec((1, *shared.shape[1:]), lambda p, w: (p, 0, 0)),
            ],
            out_specs=pl.BlockSpec((part, blocks * width), lambda p, w: (0, 0)),
            scratch_shapes=[pltpu.VMEM((part, blocks * width), F32)],
        ),
        out_shape=jax.ShapeDtypeStruct((part, blocks * width), BF16),
        cost_estimate=pl.CostEstimate(
            flops=200_000_000, bytes_accessed=4_000_000, transcendentals=300_000
        ),
    )(place, tiles, shared)


def route(expert_input, expert_gain, routes, route_weight):
    tokens, features = expert_input.shape
    count_ep = lax.axis_size(EP)
    cap = min(tokens, max(2, (9 * tokens + 4 * count_ep - 1) // (4 * count_ep)))
    return pl.pallas_call(
        partial(route_kernel, cap),
        out_shape=(
            jax.ShapeDtypeStruct((count_ep * cap, features), BF16),
            jax.ShapeDtypeStruct((count_ep * cap, 2 * tokens), BF16),
        ),
        cost_estimate=pl.CostEstimate(
            flops=200_000_000, bytes_accessed=2_000_000, transcendentals=0
        ),
    )(expert_input, expert_gain[None], routes.T, route_weight.T)


def exchanged(rows):
    count, features = rows.shape
    size = lax.axis_size(EP)
    tiles = rows.reshape(size, count // size, features // LANES, LANES)
    return lax.all_to_all(tiles, EP, 0, 0, tiled=True).reshape(count, features)


def experts(arrived, gate_weight, up_weight, down_weight):
    gate_local, up_local, down_local = gate_weight[0], up_weight[0], down_weight[0]
    count = arrived.shape[0] // CHUNKS
    gathered = [ring_gather(arrived[c * count : (c + 1) * count]) for c in range(CHUNKS)]
    sums = []
    for pieces in gathered:
        piece = jnp.concatenate(pieces, axis=0)
        upward = jnp.dot(piece, up_local, preferred_element_type=F32)
        gate = jnp.dot(piece, gate_local, preferred_element_type=F32)
        hidden = (jax.nn.silu(gate) * upward).astype(BF16)
        result = jnp.dot(hidden, down_local, preferred_element_type=F32).astype(BF16)
        ends, total = [], 0
        for p in pieces[:-1]:
            total += p.shape[0]
            ends.append(total)
        sums.append(ring_sum(*jnp.split(result, ends)))
    return jnp.concatenate(sums)


def body(
    query_plain,
    query_rotary,
    latent_input,
    rotary_key,
    key_weight,
    value_weight,
    latent_gain,
    head_gain,
    out_weight,
    expert_input,
    expert_gain,
    routes,
    route_weight,
    gate_weight,
    up_weight,
    down_weight,
):
    tokens = query_plain.shape[0]
    heads = key_weight.shape[1] // PLAIN_DIM
    outgoing, shares = route(expert_input, expert_gain, routes, route_weight)
    outgoing, query_plain, query_rotary, latent_input, rotary_key = lax.optimization_barrier(
        (outgoing, query_plain, query_rotary, latent_input, rotary_key)
    )
    arrived = exchanged(outgoing)
    every, shared = prepare(
        query_plain,
        query_rotary,
        latent_input,
        rotary_key,
        key_weight,
        value_weight,
        latent_gain,
        head_gain,
        out_weight,
    )
    sums = experts(arrived, gate_weight, up_weight, down_weight)
    sums, every, shared = lax.optimization_barrier((sums, every, shared))
    returned = exchanged(sums)
    attended = attend(every, shared, tokens, heads)
    combined = lax.dot_general(
        shares, returned, (((0,), (0,)), ((), ())), preferred_element_type=F32
    )
    rows = expert_input.shape[0]
    return (attended, (combined[:rows] + combined[rows:]).astype(BF16))


def solution(mesh):
    finer = Mesh(
        mesh.devices.reshape(mesh.shape["grp"], 16, 2, mesh.shape["tp"]),
        ("grp", "ep_0", "ep_1", "tp"),
    )
    in_specs = (
        P(GRP_EP, "tp"),
        P(GRP_EP, "tp"),
        P(GRP_EP, None),
        P(GRP_EP, None),
        P(None, "tp"),
        P(None, "tp"),
        P(),
        P("tp"),
        P("tp", None),
        P(GRP_EP_TP, None),
        P(),
        P(GRP_EP_TP, None),
        P(GRP_EP_TP, None),
        P(EP, None, "tp"),
        P(EP, None, "tp"),
        P(EP, "tp", None),
    )
    out_specs = (P(GRP_EP_TP, None), P(GRP_EP_TP, None))
    return jax.shard_map(body, mesh=finer, in_specs=in_specs, out_specs=out_specs, check_vma=False)
```

```python
from functools import partial

import jax
import jax.numpy as jnp
from jax import lax
from jax.experimental import pallas as pl
from jax.experimental.pallas import tpu as pltpu
from jax.sharding import Mesh
from jax.sharding import PartitionSpec as P


PLAIN_DIM = 64
ROTARY_DIM = 32
VALUE_DIM = 64
TOP = 2
LANES = 128
EP = ("ep_0", "ep_1")
GRP_EP = ("grp", "ep_0", "ep_1")
GRP_EP_TP = ("grp", "ep_0", "ep_1", "tp")

CHUNKS = 2
EPSILON = 1e-06
THETA = 10000.0
BF16 = jnp.bfloat16
F32 = jnp.float32


def normalize(entries, gain):
    wide = entries.astype(F32)
    factor = lax.rsqrt(jnp.mean(wide * wide, axis=-1, keepdims=True) + EPSILON)
    return wide * factor * gain.astype(F32)


def rotate(entries, positions):
    half = entries.shape[-1] // 2
    freqs = THETA ** (-jnp.arange(half, dtype=F32) / half)
    angle = positions.astype(F32)[:, None, None] * freqs[None, None, :]
    cosine = jnp.cos(angle)
    sine = jnp.sin(angle)
    first = entries[..., :half].astype(F32)
    second = entries[..., half:].astype(F32)
    turned = jnp.concatenate(
        [first * cosine - second * sine, first * sine + second * cosine], axis=-1
    )
    return turned.astype(BF16)


def ring(step):
    size = lax.axis_size("tp")
    return [(i, (i + step) % size) for i in range(size)]


def ring_gather(own):
    cut = (own.shape[0] // 2 + 7) // 8 * 8
    from_left = lax.ppermute(own, "tp", ring(1))
    from_right = lax.ppermute(own, "tp", ring(-1))
    far_low = lax.ppermute(from_left[:cut], "tp", ring(1))
    far_high = lax.ppermute(from_right[cut:], "tp", ring(-1))
    return own, from_left, from_right, far_low, far_high


def ring_sum(own, to_left, to_right, far_low, far_high):
    cut = far_low.shape[0]
    low = lax.ppermute(far_low, "tp", ring(-1))
    high = lax.ppermute(far_high, "tp", ring(1))
    send_left = jnp.concatenate(
        [(to_left[:cut].astype(F32) + low.astype(F32)).astype(BF16), to_left[cut:]]
    )
    send_right = jnp.concatenate(
        [to_right[:cut], (to_right[cut:].astype(F32) + high.astype(F32)).astype(BF16)]
    )
    a = lax.ppermute(send_left, "tp", ring(-1))
    b = lax.ppermute(send_right, "tp", ring(1))
    return (own.astype(F32) + a.astype(F32) + b.astype(F32)).astype(BF16)


def attention_kernel(where_ref, latent_ref, head_ref, out_ref, score_ref, both_ref):
    span = 512
    ep, part, quarter = where_ref[0], where_ref[1], where_ref[2]
    rows = head_ref.shape[1]
    per = span // 64
    weights = head_ref[0, :, :LANES]
    query = head_ref[0, :, LANES:]
    factor = (PLAIN_DIM + ROTARY_DIM) ** (-0.5) * 1.4426950408889634
    last = ep // per
    lane = lax.broadcasted_iota(jnp.int32, (span, LANES), 1)

    def scored(i):
        begin = pl.multiple_of(i * span, span)
        both = jnp.dot(
            latent_ref[pl.ds(begin, span), : 2 * LANES], weights, preferred_element_type=F32
        ).astype(BF16)
        both_ref[pl.ds(begin, span), :] = both
        keys = jnp.where(lane < PLAIN_DIM, both, latent_ref[pl.ds(begin, span), 2 * LANES :])
        return (
            lax.dot_general(query, keys, (((1,), (1,)), ((), ())), preferred_element_type=F32)
            * factor
        )

    def first(i, highest):
        scores = scored(i)
        score_ref[:, pl.ds(pl.multiple_of(i * span, span), span)] = scores
        return jnp.maximum(highest, jnp.max(scores, axis=-1, keepdims=True))

    highest = lax.fori_loop(0, last, first, jnp.full((rows, 1), -1e30, F32))
    scores = scored(last)
    column = lax.broadcasted_iota(jnp.int32, (rows, span), 1)
    line = lax.broadcasted_iota(jnp.int32, (rows, span), 0)
    key_place = (column // 64 + last * per) * quarter + part * 64 + column % 64
    scores = jnp.where(key_place <= line + ep * quarter, scores, -1e30)
    score_ref[:, pl.ds(pl.multiple_of(last * span, span), span)] = scores
    highest = jnp.maximum(highest, jnp.max(scores, axis=-1, keepdims=True))

    def second(i, total):
        begin = pl.multiple_of(i * span, span)
        kept = jnp.exp2(score_ref[:, pl.ds(begin, span)] - highest).astype(BF16)
        return total + jnp.dot(kept, both_ref[pl.ds(begin, span), :], preferred_element_type=F32)

    total = lax.fori_loop(0, last + 1, second, jnp.zeros((rows, LANES), F32))
    wide = lax.broadcasted_iota(jnp.int32, (rows, LANES), 1)
    out_ref[...] = jnp.where(wide < PLAIN_DIM, jnp.broadcast_to(highest, (rows, LANES)), total)


def finish_kernel(where_ref, tiles_ref, shared_ref, out_ref, total_ref):
    p = pl.program_id(0)
    rows = tiles_ref.shape[1]
    lines = LANES
    start = shared_ref.shape[1] - 16
    width = shared_ref.shape[2]
    blocks = out_ref.shape[1] // width
    lane = lax.broadcasted_iota(jnp.int32, (rows, LANES), 1)
    outputs = []
    for h in range(2):
        block = tiles_ref[:, :, h * LANES : (h + 1) * LANES]
        peaks = [pltpu.roll(block[i], PLAIN_DIM, 1) for i in range(block.shape[0])]
        top = peaks[0]
        for other in peaks[1:]:
            top = jnp.maximum(top, other)
        context = jnp.zeros((rows, LANES), F32)
        for i, peak in enumerate(peaks):
            context = context + block[i] * jnp.exp2(peak - top)
        context = jnp.where(lane < PLAIN_DIM, 0.0, context)
        mean = jnp.sum(context * context, axis=-1, keepdims=True) / VALUE_DIM
        gain = shared_ref[0, start : start + 16, h * LANES : (h + 1) * LANES].astype(F32)[:1]
        outputs.append(context * lax.rsqrt(mean + EPSILON) * gain)
    head_output = jnp.where(
        lane < PLAIN_DIM, pltpu.roll(outputs[0], PLAIN_DIM, 1), outputs[1]
    ).astype(BF16)
    for i in range(blocks):
        at = start - (blocks - i) * lines
        share = jnp.dot(
            head_output, shared_ref[0, at : at + lines, :], preferred_element_type=F32
        ).astype(BF16).astype(F32)
        cut = slice(i * width, (i + 1) * width)

        @pl.when(p == 0)
        def _():
            total_ref[:, cut] = share

        @pl.when(p > 0)
        def _():
            total_ref[:, cut] = total_ref[:, cut] + share

    @pl.when(p == pl.num_programs(0) - 1)
    def _():
        out_ref[...] = total_ref[...].astype(BF16)


def route_kernel(cap, input_ref, gain_ref, route_ref, weight_ref, rows_ref, shares_ref):
    tokens = input_ref.shape[0]
    wide = input_ref[...].astype(F32)
    factor = lax.rsqrt(jnp.mean(wide * wide, axis=-1, keepdims=True) + EPSILON)
    normed = (wide * factor * gain_ref[...].astype(F32)).astype(BF16)
    slots = rows_ref.shape[0]
    ids = lax.broadcasted_iota(jnp.int32, (slots // cap, tokens), 0)
    named = [ids == route_ref[k : k + 1, :] for k in range(TOP)]
    onehot = jnp.where(named[0] | named[1], 1.0, 0.0).astype(BF16)
    line = lax.broadcasted_iota(jnp.int32, (tokens, tokens), 0)
    column = lax.broadcasted_iota(jnp.int32, (tokens, tokens), 1)
    before = jnp.where(line < column, 1.0, 0.0).astype(BF16)
    earlier = jnp.dot(onehot, before, preferred_element_type=F32)
    slot = lax.broadcasted_iota(jnp.int32, (slots, tokens), 0)
    selection = jnp.zeros((slots, tokens), F32)
    shares = jnp.zeros((slots, tokens), F32)
    for k in range(TOP):
        rank = jnp.sum(jnp.where(named[k], earlier, 0.0), axis=0, keepdims=True)
        hit = slot == route_ref[k : k + 1, :] * cap + rank.astype(jnp.int32)
        selection = selection + jnp.where(hit, 1.0, 0.0)
        shares = shares + jnp.where(hit, weight_ref[k : k + 1, :], 0.0)
    coarse = shares.astype(BF16)
    shares_ref[:, :tokens] = coarse
    shares_ref[:, tokens:] = (shares - coarse.astype(F32)).astype(BF16)
    rows_ref[...] = jnp.dot(
        selection.astype(BF16), normed, preferred_element_type=F32
    ).astype(BF16)


def prepare(
    query_plain,
    query_rotary,
    latent_input,
    rotary_key,
    key_weight,
    value_weight,
    latent_gain,
    head_gain,
    out_weight,
):
    tokens = query_plain.shape[0]
    heads = key_weight.shape[1] // PLAIN_DIM
    count_tp = lax.axis_size("tp")
    part = tokens // count_tp
    ep = lax.axis_index(EP)
    offset = ep * tokens
    positions = offset + jnp.arange(tokens, dtype=jnp.int32)
    begin = lax.axis_index("tp") * part
    own_latent = normalize(
        lax.dynamic_slice_in_dim(latent_input, begin, part, 0), latent_gain
    ).astype(BF16)
    own_rotated = rotate(
        lax.dynamic_slice_in_dim(rotary_key, begin, part, 0).reshape(part, 1, ROTARY_DIM),
        offset + begin + jnp.arange(part, dtype=jnp.int32),
    ).reshape(part, ROTARY_DIM)
    margin = LANES - PLAIN_DIM - ROTARY_DIM
    own = jnp.concatenate(
        [own_latent, jnp.pad(own_rotated, ((0, 0), (PLAIN_DIM, margin)))], axis=1
    )
    count = lax.axis_size("ep_0")
    copies = jnp.broadcast_to(own[None], (count, *own.shape))
    lane = lax.all_to_all(copies, "ep_0", 0, 0, tiled=True)
    other = lax.ppermute(lane, "ep_1", [(0, 1), (1, 0)])
    first = lax.axis_index("ep_1") == 0
    every = jnp.stack([jnp.where(first, lane, other), jnp.where(first, other, lane)], axis=1)
    every = every.reshape(-1, own.shape[1])

    query_rotated = rotate(query_rotary.reshape(tokens, heads, ROTARY_DIM), positions)
    pieces = []
    for h in range(heads):
        cut = slice(h * PLAIN_DIM, (h + 1) * PLAIN_DIM)
        pieces += [
            key_weight[:, cut],
            value_weight[:, cut],
            query_plain[:, cut],
            query_rotated[:, h],
            jnp.zeros((tokens, margin), BF16),
        ]
    packed = jnp.concatenate(pieces, axis=1)
    width = packed.shape[1]
    blocks = out_weight.shape[1] // width
    gains = jnp.zeros((16, width), BF16)
    for h in range(heads):
        cut = slice(h * PLAIN_DIM, (h + 1) * PLAIN_DIM)
        place = slice(h * LANES + PLAIN_DIM, (h + 1) * LANES)
        gains = gains.at[:, place].set(jnp.broadcast_to(head_gain[cut], (16, PLAIN_DIM)))
    packed = jnp.concatenate(
        [packed] + [out_weight[:, i * width : (i + 1) * width] for i in range(blocks)] + [gains]
    )
    shared = jnp.concatenate(ring_gather(packed)).reshape(count_tp, *packed.shape)
    return every, shared


def attend(every, shared, tokens, heads):
    count_tp = shared.shape[0]
    width = shared.shape[2]
    part = tokens // count_tp
    blocks = (shared.shape[1] - tokens - 16) // LANES
    ep = lax.axis_index(EP)
    all_heads = heads * count_tp
    me = lax.axis_index("tp")
    order = [me] + [(me + i) % count_tp for i in (-1, 1, 2)]
    place = jnp.stack([ep, me, jnp.int32(tokens)] + order).astype(jnp.int32)
    attention = pl.pallas_call(
        attention_kernel,
        grid_spec=pltpu.PrefetchScalarGridSpec(
            num_scalar_prefetch=1,
            grid=(all_heads,),
            in_specs=[
                pl.BlockSpec(every.shape, lambda h, w: (0, 0)),
                pl.BlockSpec((1, tokens, 2 * LANES), lambda h, w: (h // heads, 0, h % heads)),
            ],
            out_specs=pl.BlockSpec(
                (tokens, LANES), lambda h, w: (0, w[3 + h // heads] * heads + h % heads)
            ),
            scratch_shapes=[
                pltpu.VMEM((tokens, every.shape[0]), F32),
                pltpu.VMEM((every.shape[0], LANES), BF16),
            ],
        ),
        out_shape=jax.ShapeDtypeStruct((tokens, all_heads * LANES), F32),
        cost_estimate=pl.CostEstimate(
            flops=12_000_000_000, bytes_accessed=8_000_000, transcendentals=4_000_000
        ),
    )
    sums = attention(place, every, shared)
    tiles = sums.reshape(count_tp, part, -1)

    def block(step):
        return lax.dynamic_slice_in_dim(tiles, (me + step) % count_tp, 1, 0)

    sent = [lax.ppermute(block(i), "tp", ring(i)) for i in (1, -1, 2)]
    tiles = jnp.concatenate([block(0)] + sent)
    return pl.pallas_call(
        finish_kernel,
        grid_spec=pltpu.PrefetchScalarGridSpec(
            num_scalar_prefetch=1,
            grid=(count_tp,),
            in_specs=[
                pl.BlockSpec((count_tp, part, heads * LANES), lambda p, w: (0, 0, w[3 + p])),
                pl.BlockSpec((1, *shared.shape[1:]), lambda p, w: (p, 0, 0)),
            ],
            out_specs=pl.BlockSpec((part, blocks * width), lambda p, w: (0, 0)),
            scratch_shapes=[pltpu.VMEM((part, blocks * width), F32)],
        ),
        out_shape=jax.ShapeDtypeStruct((part, blocks * width), BF16),
        cost_estimate=pl.CostEstimate(
            flops=200_000_000, bytes_accessed=4_000_000, transcendentals=300_000
        ),
    )(place, tiles, shared)


def route(expert_input, expert_gain, routes, route_weight):
    tokens, features = expert_input.shape
    count_ep = lax.axis_size(EP)
    cap = min(tokens, max(2, (9 * tokens + 4 * count_ep - 1) // (4 * count_ep)))
    return pl.pallas_call(
        partial(route_kernel, cap),
        out_shape=(
            jax.ShapeDtypeStruct((count_ep * cap, features), BF16),
            jax.ShapeDtypeStruct((count_ep * cap, 2 * tokens), BF16),
        ),
        cost_estimate=pl.CostEstimate(
            flops=200_000_000, bytes_accessed=2_000_000, transcendentals=0
        ),
    )(expert_input, expert_gain[None], routes.T, route_weight.T)


def exchanged(rows):
    count, features = rows.shape
    size = lax.axis_size(EP)
    tiles = rows.reshape(size, count // size, features // LANES, LANES)
    return lax.all_to_all(tiles, EP, 0, 0, tiled=True).reshape(count, features)


def experts(arrived, gate_weight, up_weight, down_weight):
    gate_local, up_local, down_local = gate_weight[0], up_weight[0], down_weight[0]
    count = arrived.shape[0] // CHUNKS
    gathered = [ring_gather(arrived[c * count : (c + 1) * count]) for c in range(CHUNKS)]
    sums = []
    for pieces in gathered:
        piece = jnp.concatenate(pieces, axis=0)
        upward = jnp.dot(piece, up_local, preferred_element_type=F32)
        gate = jnp.dot(piece, gate_local, preferred_element_type=F32)
        hidden = (jax.nn.silu(gate) * upward).astype(BF16)
        result = jnp.dot(hidden, down_local, preferred_element_type=F32).astype(BF16)
        ends, total = [], 0
        for p in pieces[:-1]:
            total += p.shape[0]
            ends.append(total)
        sums.append(ring_sum(*jnp.split(result, ends)))
    return jnp.concatenate(sums)


def body(
    query_plain,
    query_rotary,
    latent_input,
    rotary_key,
    key_weight,
    value_weight,
    latent_gain,
    head_gain,
    out_weight,
    expert_input,
    expert_gain,
    routes,
    route_weight,
    gate_weight,
    up_weight,
    down_weight,
):
    tokens = query_plain.shape[0]
    heads = key_weight.shape[1] // PLAIN_DIM
    outgoing, shares = route(expert_input, expert_gain, routes, route_weight)
    outgoing, query_plain, query_rotary, latent_input, rotary_key = lax.optimization_barrier(
        (outgoing, query_plain, query_rotary, latent_input, rotary_key)
    )
    arrived = exchanged(outgoing)
    every, shared = prepare(
        query_plain,
        query_rotary,
        latent_input,
        rotary_key,
        key_weight,
        value_weight,
        latent_gain,
        head_gain,
        out_weight,
    )
    sums = experts(arrived, gate_weight, up_weight, down_weight)
    sums, shared = lax.optimization_barrier((sums, shared))
    returned = exchanged(sums)
    attended = attend(every, shared, tokens, heads)
    combined = lax.dot_general(
        shares, returned, (((0,), (0,)), ((), ())), preferred_element_type=F32
    )
    rows = expert_input.shape[0]
    return (attended, (combined[:rows] + combined[rows:]).astype(BF16))


def solution(mesh):
    finer = Mesh(
        mesh.devices.reshape(mesh.shape["grp"], 16, 2, mesh.shape["tp"]),
        ("grp", "ep_0", "ep_1", "tp"),
    )
    in_specs = (
        P(GRP_EP, "tp"),
        P(GRP_EP, "tp"),
        P(GRP_EP, None),
        P(GRP_EP, None),
        P(None, "tp"),
        P(None, "tp"),
        P(),
        P("tp"),
        P("tp", None),
        P(GRP_EP_TP, None),
        P(),
        P(GRP_EP_TP, None),
        P(GRP_EP_TP, None),
        P(EP, None, "tp"),
        P(EP, None, "tp"),
        P(EP, "tp", None),
    )
    out_specs = (P(GRP_EP_TP, None), P(GRP_EP_TP, None))
    return jax.shard_map(body, mesh=finer, in_specs=in_specs, out_specs=out_specs, check_vma=False)
```
